256 devices in a mesh: ep: 32 (over z, x), tp: 8 (over y, core).
Axes of the slice: x: 4, y: 4, z: 8, core: 2. Of those that a mesh axis runs over, the one named last changes fastest.
Arguments:
- tokens: bfloat16 [3072, 4096], P('ep'), may hold values from -6 to 6
- mix_gain: float32 [4096], replicated, may hold values from 0.1 to 1.9
- ffn_gain: float32 [4096], replicated, may hold values from 0.1 to 1.9
- in_proj: bfloat16 [4096, 1024], P(None, 'tp'), may hold values from -0.09375 to 0.09375
- decay_rate: float32 [64, 64], P('tp'), may hold values from 0.05 to 2
- frequency: float32 [64, 64], P('tp'), may hold values from -3 to 3
- log_step: float32 [64], P('tp'), may hold values from -3 to 0.5
- b_real: float32 [64, 64, 16], P('tp'), may hold values from -1.5 to 1.5
- b_imag: float32 [64, 64, 16], P('tp'), may hold values from -1.5 to 1.5
- c_real: float32 [64, 16, 64], P('tp'), may hold values from -0.75 to 0.75
- c_imag: float32 [64, 16, 64], P('tp'), may hold values from -0.75 to 0.75
- skip_gain: float32 [1024], P('tp'), may hold values from -5 to 5
- states: float32 [2, 3072, 4096], P(None, 'ep', 'tp'), may hold values from -6 to 6
- out_proj: bfloat16 [1024, 4096], P('tp'), may hold values from -0.1875 to 0.1875
- route_ids: int32 [3072, 2], P('ep'), may hold values from 0 to 31, all different within a row; in each aligned block of 96 rows (0 to 95, 96 to 191, ...) at most 12 rows name the same one
- route_logits: float32 [3072, 2], P('ep'), may hold values from -5 to 5
- expert_gate: bfloat16 [32, 4096, 3072], P('ep', None, 'tp'), may hold values from -0.09375 to 0.09375
- expert_up: bfloat16 [32, 4096, 3072], P('ep', None, 'tp'), may hold values from -0.09375 to 0.09375
- expert_down: bfloat16 [32, 3072, 4096], P('ep', 'tp'), may hold values from -0.109375 to 0.109375
- dense_gate: bfloat16 [4096, 6144], P('tp', 'ep'), may hold values from -0.09375 to 0.09375
- dense_up: bfloat16 [4096, 6144], P('tp', 'ep'), may hold values from -0.09375 to 0.09375
- dense_down: bfloat16 [6144, 4096], P('ep', 'tp'), may hold values from -0.078125 to 0.078125
- branch_gate: bfloat16 [4096], replicated, may hold values from -0.09375 to 0.09375
Outputs:
- output: bfloat16 [3072, 4096], P('ep', 'tp')
- new_states: float32 [2, 3072, 4096], P(None, 'ep', 'tp')
The draws below stay inside these ranges and needn't reach their ends.
Inputs may be any that keep to these rules, and one draw needn't show every extreme that they name: `route_ids`: each row names 2 different experts; among the rows of one device (aligned blocks of 96 rows) no expert is named by more than 12 rows.
All inputs are finite; a program needn't handle non-finite values.
Results may differ from the reference program's by a relative error of at most 0.017.
Values may be sent and summed in bfloat16 or wider, within the bound.
No kernel may reach another device: no remote copies, remote signals or barrier semaphores. Data moves between devices by JAX's collectives and lax.ppermute only.
A program may use at most 128 MiB of HBM per device.

```python
import math
import jax
import jax.numpy as jnp
import numpy as np
from jax import lax

D = 4096
S5W = 1024
GROUP = 16
GROUPS = 64
STATE = 64
FFE = 3072
FFD = 6144
TOPK = 2
SEQ_DEV = 96
BATCH = 3072
EXPERTS = 32
CAP = 12
N_EP = 32
N_TP = 8


def steps_of(own_key, dims, cuts, least, top_value):
    loudness, own = 1.0, jax.random.fold_in(own_key, 6)
    for axis_at, blocks in cuts:
        steps = jnp.exp(jax.random.uniform(jax.random.fold_in(own, axis_at), (blocks,), jnp.float32, least / len(cuts), top_value / len(cuts)))
        loudness = loudness * jnp.repeat(steps, dims[axis_at] // blocks).reshape([-1 if axis == axis_at else 1 for axis in range(len(dims))])
    return loudness


def deal_out(key, own, number, rows, number_of, top, bound, slope):
    sequence = jax.random.permutation(key, number_of)
    crowded, ordinary = portions_of(number_of, rows * top, bound, slope, True), portions_of(number_of, rows * top, bound, slope, False)
    places = jnp.arange(number_of)

    def named(lengths, turn):
        used = int((lengths > 0).sum())
        fixed = max(1, used // 4)
        passed = fixed + (places - fixed + turn * (used - fixed)) % max(1, number_of - fixed)
        return jnp.zeros((number_of,), jnp.int32).at[sequence[jnp.where(places < fixed, places, passed)]].set(jnp.asarray(lengths, jnp.int32))

    lengths = jnp.where(number % 4 == 0, named(crowded, number // 4), named(ordinary, number - number // 4 - 1))
    mixed = jax.random.permutation(jax.random.fold_in(own, 3), number_of)
    donor, receiver = mixed[0:number_of // 2 * 2:2], mixed[1:number_of // 2 * 2:2]
    slack = jnp.minimum(lengths[donor] - 1, bound - lengths[receiver]) // 2
    slack = jnp.where((donor == sequence[0]) | (receiver == sequence[0]) | (lengths[receiver] == 0), 0, jnp.maximum(slack, 0))
    passed = jax.random.randint(jax.random.fold_in(own, 4), (number_of // 2,), 0, 1 << 20) % (slack + 1)
    lengths = lengths.at[donor].add(-passed).at[receiver].add(passed)
    labels = jnp.searchsorted(jnp.cumsum(lengths), jnp.arange(rows * top), side="right").astype(jnp.int32)
    listing = labels.reshape(top, rows).T
    listing = listing[jax.random.permutation(jax.random.fold_in(own, 1), rows)]
    turn = jax.random.randint(jax.random.fold_in(own, 2), (rows, 1), 0, top)
    return jnp.take_along_axis(listing, (jnp.arange(top)[None, :] + turn) % top, axis=1)


def portions_of(amount, total, bound, slope, full):
    weights = [(1 << 20) // math.isqrt(standing ** slope) + 1 for standing in range(1, amount + 1)]
    largest = bound if full else min(bound, max(-(-total // amount), total * weights[0] // sum(weights)))
    least = 1 if total - largest >= amount - 1 else 0
    counts, rest = [largest] + [least] * (amount - 1), total - largest - least * (amount - 1)
    while rest > 0:
        free = [i for i in range(1, amount) if counts[i] < largest] or [i for i in range(1, amount) if counts[i] < bound]
        mass, budget = sum([weights[i] for i in free]), rest
        for i in free:
            addition = min(bound - counts[i], max(1, budget * weights[i] // mass), rest)
            counts[i] = counts[i] + addition
            rest = rest - addition
    return np.array(counts)


def noise(rng, extent, width, bound, pieces=(), kind=jnp.bfloat16):
    loudness = steps_of(rng, extent, pieces, -0.22, 0.18) if pieces else 1.0
    values = jax.random.normal(rng, extent, jnp.float32) * width * loudness
    return jnp.minimum(jnp.maximum(values, -bound), bound).astype(kind)


def setup_inputs(seed: int = 0) -> dict:
    seeds = jax.random.split(jax.random.key(seed), 24)
    tokens = noise(seeds[0], (BATCH, D), 1.0, 6.0, ((0, 32),))
    mix_gain = jnp.clip(1.0 + 0.18 * jax.random.normal(seeds[1], (D,), jnp.float32), 0.1, 1.9)
    ffn_gain = jnp.clip(1.0 + 0.18 * jax.random.normal(seeds[2], (D,), jnp.float32), 0.1, 1.9)
    in_proj = noise(seeds[3], (D, S5W), D ** -0.5, 0.09375, ((1, 8),))
    decay_rate = jnp.clip(jnp.exp(math.log(2.0) - 3.6888794 * jax.random.uniform(seeds[4], (GROUPS, STATE), jnp.float32) ** steps_of(seeds[4], (GROUPS, STATE), ((0, 8),), -0.2, 0.2)), 0.05, 2.0)
    frequency = jnp.clip(jax.random.uniform(seeds[5], (GROUPS, STATE), jnp.float32, -3.0, 3.0) * steps_of(seeds[5], (GROUPS, STATE), ((0, 8),), -0.4, 0.0), -3.0, 3.0)
    log_step = jnp.clip(-3.0 + 3.5 * jax.random.uniform(seeds[6], (GROUPS,), jnp.float32) ** steps_of(seeds[6], (GROUPS,), ((0, 8),), -0.2, 0.2), -3.0, 0.5)
    b_real = noise(seeds[7], (GROUPS, STATE, GROUP), GROUP ** -0.5, 1.5, ((0, 8),), jnp.float32)
    b_imag = noise(seeds[8], (GROUPS, STATE, GROUP), GROUP ** -0.5, 1.5, ((0, 8),), jnp.float32)
    c_real = noise(seeds[9], (GROUPS, GROUP, STATE), STATE ** -0.5, 0.75, ((0, 8),), jnp.float32)
    c_imag = noise(seeds[10], (GROUPS, GROUP, STATE), STATE ** -0.5, 0.75, ((0, 8),), jnp.float32)
    skip_gain = noise(seeds[11], (S5W,), 1.0, 5.0, ((0, 8),), jnp.float32)
    states = noise(seeds[12], (2, BATCH, GROUPS * STATE), 1.0, 6.0, ((1, 32), (2, 8)), jnp.float32)
    out_proj = noise(seeds[13], (S5W, D), S5W ** -0.5, 0.1875, ((0, 8),))
    route_ids_keys = jax.random.split(jax.random.fold_in(seeds[14], 1), BATCH // SEQ_DEV)
    route_ids_turns = jax.random.permutation(jax.random.fold_in(seeds[14], 3), BATCH // SEQ_DEV)
    route_ids = jax.vmap(lambda own, number: deal_out(jax.random.fold_in(seeds[14], 2), own, number, SEQ_DEV, EXPERTS, TOPK, CAP, 2))(route_ids_keys, route_ids_turns).reshape((BATCH, TOPK))
    route_logits = noise(seeds[15], (BATCH, TOPK), 1.0, 5.0, ((0, 32),), jnp.float32)
    expert_gate = noise(seeds[16], (EXPERTS, D, FFE), D ** -0.5, 0.09375, ((0, 32), (2, 8)))
    expert_up = noise(seeds[17], (EXPERTS, D, FFE), D ** -0.5, 0.09375, ((0, 32), (2, 8)))
    expert_down = noise(seeds[18], (EXPERTS, FFE, D), FFE ** -0.5, 0.109375, ((0, 32), (1, 8)))
    dense_gate = noise(seeds[19], (D, FFD), D ** -0.5, 0.09375, ((0, 8), (1, 32)))
    dense_up = noise(seeds[20], (D, FFD), D ** -0.5, 0.09375, ((0, 8), (1, 32)))
    dense_down = noise(seeds[21], (FFD, D), FFD ** -0.5, 0.078125, ((0, 32), (1, 8)))
    branch_gate = noise(seeds[22], (D,), D ** -0.5, 0.09375)
    return dict(tokens=tokens, mix_gain=mix_gain, ffn_gain=ffn_gain, in_proj=in_proj, decay_rate=decay_rate, frequency=frequency, log_step=log_step, b_real=b_real, b_imag=b_imag, c_real=c_real, c_imag=c_imag, skip_gain=skip_gain, states=states, out_proj=out_proj, route_ids=route_ids, route_logits=route_logits, expert_gate=expert_gate, expert_up=expert_up, expert_down=expert_down, dense_gate=dense_gate, dense_up=dense_up, dense_down=dense_down, branch_gate=branch_gate)


def rms_norm(values, gain):
    flt = values.astype(jnp.float32)
    scaled = flt * lax.rsqrt(lax.optimization_barrier(jnp.mean(flt * flt, axis=-1, keepdims=True)) + 1e-06)
    return (scaled * gain.astype(jnp.float32)).astype(jnp.bfloat16)

def discretize(decay_rate, frequency, log_step, b_real, b_imag):
    step_size = jnp.exp(log_step)[:, None]
    lam_re = -decay_rate
    lam_im = frequency
    magnitude = jnp.exp(lam_re * step_size)
    abar_re = magnitude * jnp.cos(lam_im * step_size)
    abar_im = magnitude * jnp.sin(lam_im * step_size)
    denom = lam_re * lam_re + lam_im * lam_im
    fac_re = ((abar_re - 1.0) * lam_re + abar_im * lam_im) / denom
    fac_im = (abar_im * lam_re - (abar_re - 1.0) * lam_im) / denom
    bbar_re = fac_re[..., None] * b_real - fac_im[..., None] * b_imag
    bbar_im = fac_re[..., None] * b_imag + fac_im[..., None] * b_real
    return (abar_re, abar_im, bbar_re, bbar_im)

def state_step(drive, states, decay_rate, frequency, log_step, b_real, b_imag, c_real, c_imag, skip_gain):
    count = drive.shape[0]
    groups = decay_rate.shape[0]
    abar_re, abar_im, bbar_re, bbar_im = discretize(decay_rate, frequency, log_step, b_real, b_imag)
    grouped = drive.astype(jnp.float32).reshape(count, groups, GROUP)
    old_re = states[0].reshape(count, groups, STATE)
    old_im = states[1].reshape(count, groups, STATE)
    high = lax.Precision.HIGHEST
    push_re = jnp.einsum('ngh,gph->ngp', grouped, bbar_re, precision=high)
    push_im = jnp.einsum('ngh,gph->ngp', grouped, bbar_im, precision=high)
    new_re = abar_re * old_re - abar_im * old_im + push_re
    new_im = abar_re * old_im + abar_im * old_re + push_im
    readout = jnp.einsum('ngp,ghp->ngh', new_re, c_real, precision=high) - jnp.einsum('ngp,ghp->ngh', new_im, c_imag, precision=high) + skip_gain.reshape(groups, GROUP) * grouped
    reads = jax.nn.gelu(readout.reshape(count, groups * GROUP)).astype(jnp.bfloat16)
    fresh = jnp.stack([new_re.reshape(count, groups * STATE), new_im.reshape(count, groups * STATE)])
    return (reads, fresh)

def reference(tokens, mix_gain, ffn_gain, in_proj, decay_rate, frequency, log_step, b_real, b_imag, c_real, c_imag, skip_gain, states, out_proj, route_ids, route_logits, expert_gate, expert_up, expert_down, dense_gate, dense_up, dense_down, branch_gate):
    normed = rms_norm(tokens, mix_gain)
    drive = jnp.dot(normed, in_proj, preferred_element_type=jnp.float32).astype(jnp.bfloat16)
    reads, new_states = state_step(drive, states, decay_rate, frequency, log_step, b_real, b_imag, c_real, c_imag, skip_gain)
    block_width = S5W // N_TP
    mixed = jnp.zeros((BATCH, D), jnp.float32)
    for block in range(N_TP):
        piece = jnp.dot(reads[:, block * block_width:(block + 1) * block_width], out_proj[block * block_width:(block + 1) * block_width], preferred_element_type=jnp.float32).astype(jnp.bfloat16)
        mixed = mixed + piece.astype(jnp.float32)
    mixed = mixed.astype(jnp.bfloat16)
    resid = (tokens.astype(jnp.float32) + mixed.astype(jnp.float32)).astype(jnp.bfloat16)
    normed_two = rms_norm(resid, ffn_gain)
    route_weights = jax.nn.softmax(route_logits, axis=-1)
    blocked_ids = route_ids.reshape(N_EP, SEQ_DEV * TOPK)
    onehot = (blocked_ids[..., None] == jnp.arange(EXPERTS, dtype=jnp.int32)[None, None, :]).astype(jnp.int32)
    rank = jnp.cumsum(onehot, axis=1) - onehot
    slot = lax.optimization_barrier(jnp.sum(rank * onehot, axis=-1))
    block_index = jnp.arange(N_EP, dtype=jnp.int32)[:, None]
    position = blocked_ids * (N_EP * CAP) + block_index * CAP + slot
    token_index = block_index * SEQ_DEV + jnp.arange(SEQ_DEV * TOPK, dtype=jnp.int32)[None, :] // TOPK
    table = jnp.full((EXPERTS * N_EP * CAP,), BATCH, jnp.int32).at[position.reshape(-1)].set(token_index.reshape(-1))
    padded = jnp.concatenate([normed_two, jnp.zeros((1, D), jnp.bfloat16)], axis=0)
    hidden_block = FFE // N_TP

    def one_expert(inputs):
        index_row, gate_w, up_w, down_w = inputs
        rows_in = padded[index_row]
        summed = jnp.zeros((N_EP * CAP, D), jnp.float32)
        for block in range(N_TP):
            lo = block * hidden_block
            gate_val = jnp.dot(rows_in, gate_w[:, lo:lo + hidden_block], preferred_element_type=jnp.float32)
            up_val = jnp.dot(rows_in, up_w[:, lo:lo + hidden_block], preferred_element_type=jnp.float32)
            hidden = (jax.nn.silu(gate_val) * up_val).astype(jnp.bfloat16)
            piece = jnp.dot(hidden, down_w[lo:lo + hidden_block], preferred_element_type=jnp.float32)
            summed = summed + piece.astype(jnp.bfloat16).astype(jnp.float32)
        return summed.astype(jnp.bfloat16)
    expert_out = lax.map(one_expert, (table.reshape(EXPERTS, N_EP * CAP), expert_gate, expert_up, expert_down))
    picked = expert_out.reshape(EXPERTS * N_EP * CAP, D)[position.reshape(-1)]
    picked = picked.reshape(BATCH, TOPK, D).astype(jnp.float32)
    routed = lax.optimization_barrier(jnp.sum(route_weights[..., None] * picked, axis=1))
    gate_val = jnp.dot(normed_two, dense_gate, preferred_element_type=jnp.float32)
    up_val = jnp.dot(normed_two, dense_up, preferred_element_type=jnp.float32)
    dense_hidden = (jax.nn.silu(gate_val) * up_val).astype(jnp.bfloat16)
    dense_term = jnp.dot(dense_hidden, dense_down, preferred_element_type=jnp.float32)
    branch = jax.nn.sigmoid(jnp.dot(normed_two, branch_gate, preferred_element_type=jnp.float32))
    output = (resid.astype(jnp.float32) + routed + branch[:, None] * dense_term).astype(jnp.bfloat16)
    return (output, new_states)
```

```python
import jax
import jax.numpy as jnp
from jax import lax
from jax.sharding import Mesh
from jax.sharding import PartitionSpec as P

GROUP = 16
STATE = 64
EP = ("z", "x")
TP = ("y", "c")
PAD = 16
F32 = jnp.float32
BF16 = jnp.bfloat16


def fetch(x, axis, ahead):
    peers = lax.axis_size(axis)
    return lax.ppermute(x, axis, [((i + ahead) % peers, i) for i in range(peers)])


def tp_block(ahead, other):
    chip = lax.rem(lax.axis_index("y") + ahead, lax.axis_size("y"))
    core = lax.axis_index("c")
    return chip * 2 + ((1 - core) if other else core)


def tp_reduce_scatter(block_of):
    sums = {}
    for ahead in (2, 1, 3, 0):
        mine = block_of(tp_block(ahead, False))
        swapped = fetch(block_of(tp_block(ahead, True)), "c", 1)
        sums[ahead] = mine.astype(F32) + swapped.astype(F32)
    total = sums[0]
    for ahead in (2, 1, 3):
        total = total + fetch(sums[ahead].astype(BF16), "y", 4 - ahead).astype(F32)
    return total


def tp_blocks(own):
    yield tp_block(0, False), own
    yield tp_block(0, True), fetch(own, "c", 1)
    arrived = [(ahead, fetch(own, "y", ahead)) for ahead in (1, 3, 2)]
    for ahead, block in arrived:
        yield tp_block(ahead, False), block
        yield tp_block(ahead, True), fetch(block, "c", 1)


def tp_sum_small(x):
    x = x + fetch(x, "c", 1)
    return x + fetch(x, "y", 1) + fetch(x, "y", 2) + fetch(x, "y", 3)


def rms_norm(values, gain):
    flt = values.astype(F32)
    scaled = flt * lax.rsqrt(jnp.mean(flt * flt, axis=-1, keepdims=True) + 1e-06)
    return (scaled * gain).astype(BF16)


def discretize(decay_rate, frequency, log_step, b_real, b_imag):
    step_size = jnp.exp(log_step)[:, None]
    lam_re = -decay_rate
    magnitude = jnp.exp(lam_re * step_size)
    abar_re = magnitude * jnp.cos(frequency * step_size)
    abar_im = magnitude * jnp.sin(frequency * step_size)
    denom = lam_re * lam_re + frequency * frequency
    fac_re = ((abar_re - 1.0) * lam_re + abar_im * frequency) / denom
    fac_im = (abar_im * lam_re - (abar_re - 1.0) * frequency) / denom
    bbar_re = fac_re[..., None] * b_real - fac_im[..., None] * b_imag
    bbar_im = fac_re[..., None] * b_imag + fac_im[..., None] * b_real
    return (abar_re, abar_im, bbar_re, bbar_im)


def state_step(
    drive, states, decay_rate, frequency, log_step, b_real, b_imag, c_real, c_imag, skip_gain
):
    count = drive.shape[0]
    groups = decay_rate.shape[0]
    abar_re, abar_im, bbar_re, bbar_im = discretize(decay_rate, frequency, log_step, b_real, b_imag)
    grouped = drive.astype(F32).reshape(count, groups, GROUP)
    old_re = states[0].reshape(count, groups, STATE)
    old_im = states[1].reshape(count, groups, STATE)
    push_re = jnp.einsum("ngh,gph->ngp", grouped, bbar_re)
    push_im = jnp.einsum("ngh,gph->ngp", grouped, bbar_im)
    new_re = abar_re * old_re - abar_im * old_im + push_re
    new_im = abar_re * old_im + abar_im * old_re + push_im
    readout = (
        jnp.einsum("ngp,ghp->ngh", new_re, c_real)
        - jnp.einsum("ngp,ghp->ngh", new_im, c_imag)
        + skip_gain.reshape(groups, GROUP) * grouped
    )
    reads = jax.nn.gelu(readout.reshape(count, groups * GROUP)).astype(BF16)
    fresh = jnp.stack(
        [new_re.reshape(count, groups * STATE), new_im.reshape(count, groups * STATE)]
    )
    return (reads, fresh)


def shards(
    tokens,
    mix_gain,
    ffn_gain,
    in_proj,
    decay_rate,
    frequency,
    log_step,
    b_real,
    b_imag,
    c_real,
    c_imag,
    skip_gain,
    states,
    out_proj,
    route_ids,
    route_logits,
    expert_gate,
    expert_up,
    expert_down,
    dense_gate,
    dense_up,
    dense_down,
    branch_gate,
):
    seq_count, width = tokens.shape
    tp_count = lax.axis_size(TP)
    ep_count = lax.axis_size(EP)
    z_count = lax.axis_size("z")
    tp_index = lax.axis_index(TP)
    part = width // tp_count
    cap = max(2, 2 * seq_count * route_ids.shape[1] // ep_count)
    own_start = tp_index * part

    both = jnp.concatenate([dense_gate, dense_up], axis=1)
    hidden = dense_gate.shape[1]
    both_all = lax.all_gather(both, "z", axis=0)
    down_all = lax.all_gather(dense_down, "z", axis=0)

    normed = rms_norm(tokens, mix_gain)
    drive = jnp.dot(normed, in_proj, preferred_element_type=F32).astype(BF16)
    reads, new_states = state_step(
        drive, states, decay_rate, frequency, log_step, b_real, b_imag, c_real, c_imag, skip_gain
    )
    partial = jnp.dot(reads, out_proj, preferred_element_type=F32).astype(BF16)
    mixed = tp_reduce_scatter(
        lambda t: lax.dynamic_slice_in_dim(partial, t * part, part, 1)
    ).astype(BF16)
    tokens_own = lax.dynamic_slice_in_dim(tokens, own_start, part, 1)
    resid = (tokens_own.astype(F32) + mixed.astype(F32)).astype(BF16)
    gain_own = lax.dynamic_slice_in_dim(ffn_gain, own_start, part, 0)

    top_count = route_ids.shape[1]
    flat_ids = route_ids.reshape(-1)
    onehot = (flat_ids[:, None] == jnp.arange(ep_count, dtype=jnp.int32)[None, :]).astype(jnp.int32)
    rank = jnp.cumsum(onehot, axis=0) - onehot
    slot = jnp.sum(rank * onehot, axis=1)
    target = flat_ids * PAD + slot
    select = target[None, :] == jnp.arange(ep_count * PAD, dtype=jnp.int32)[:, None]
    select = jnp.any(select.reshape(ep_count * PAD, seq_count, top_count), axis=2).astype(BF16)
    send = jnp.dot(select, resid, preferred_element_type=F32).astype(BF16)
    got = lax.all_to_all(
        send.reshape(ep_count, PAD, part), EP, split_axis=0, concat_axis=0, tiled=True
    )
    rows = ep_count * cap
    wide = jnp.arange(ep_count * PAD, dtype=jnp.int32)
    narrow = jnp.arange(rows, dtype=jnp.int32)
    spread = wide // PAD * cap + wide % PAD
    keep = (spread[None, :] == narrow[:, None]) & (wide % PAD < cap)[None, :]
    keep = keep.astype(BF16)
    rows_own = jnp.dot(
        keep, got.reshape(ep_count * PAD, part), preferred_element_type=F32
    ).astype(BF16)

    group = [resid] + [fetch(resid, "x", ahead) for ahead in (1, 2, 3)]
    group = jnp.concatenate(group, axis=0)
    group_flt = group.astype(F32)
    gate_vec = gain_own * lax.dynamic_slice_in_dim(branch_gate, own_start, part, 0).astype(F32)
    stats = jnp.stack([jnp.sum(group_flt * group_flt, axis=1), jnp.sum(group_flt * gate_vec, axis=1)])
    stats = tp_sum_small(stats)
    group_scale = lax.rsqrt(stats[0] / width + 1e-06)
    branch = jax.nn.sigmoid(group_scale[:seq_count] * stats[1, :seq_count])
    group_in = (group_flt * gain_own).astype(BF16)
    wide_part = jnp.stack(
        [
            jnp.dot(group_in, both_all[k], preferred_element_type=F32).astype(BF16)
            for k in range(z_count)
        ]
    )
    wide_sum = lax.psum_scatter(wide_part, TP, scatter_dimension=0, tiled=False).astype(F32)
    wide_sum = wide_sum * group_scale[:, None]
    dense_hidden = (jax.nn.silu(wide_sum[:, :hidden]) * wide_sum[:, hidden:]).astype(BF16)
    hidden_all = lax.all_gather(dense_hidden, TP, axis=0)
    dense_part = jnp.zeros((group.shape[0], part), F32)
    for k in range(z_count):
        dense_part = dense_part + jnp.dot(hidden_all[k], down_all[k], preferred_element_type=F32)
    dense_term = dense_part[:seq_count]
    for ahead in (1, 2, 3):
        piece = dense_part[ahead * seq_count : (ahead + 1) * seq_count].astype(BF16)
        dense_term = dense_term + fetch(piece, "x", 4 - ahead).astype(F32)

    gate_w, up_w, down_w = (expert_gate[0], expert_up[0], expert_down[0])
    gate_acc, up_acc, square = (0.0, 0.0, 0.0)
    for index, block in tp_blocks(rows_own):
        flt = block.astype(F32)
        square = square + jnp.sum(flt * flt, axis=1)
        scaled = (flt * lax.dynamic_slice_in_dim(ffn_gain, index * part, part, 0)).astype(BF16)
        gate_acc = gate_acc + jnp.dot(
            scaled, lax.dynamic_slice_in_dim(gate_w, index * part, part, 0), preferred_element_type=F32
        )
        up_acc = up_acc + jnp.dot(
            scaled, lax.dynamic_slice_in_dim(up_w, index * part, part, 0), preferred_element_type=F32
        )
    scale = lax.rsqrt(square / width + 1e-06)[:, None]
    hidden_e = (jax.nn.silu(gate_acc * scale) * (up_acc * scale)).astype(BF16)
    answered = tp_reduce_scatter(
        lambda t: jnp.dot(
            hidden_e,
            lax.dynamic_slice_in_dim(down_w, t * part, part, 1),
            preferred_element_type=F32,
        ).astype(BF16)
    ).astype(BF16)
    back = jnp.dot(keep.T, answered, preferred_element_type=F32).astype(BF16)
    returned = lax.all_to_all(
        back.reshape(ep_count, PAD, part), EP, split_axis=0, concat_axis=0, tiled=True
    )
    picked = returned.reshape(ep_count * PAD, part)[target]
    picked = picked.reshape(seq_count, top_count, part).astype(F32)
    route_weights = jax.nn.softmax(route_logits, axis=-1)
    routed = jnp.sum(route_weights[..., None] * picked, axis=1)
    output = (resid.astype(F32) + routed + branch[:, None] * dense_term).astype(BF16)
    return (output, new_states)


def solution(mesh):
    finer = Mesh(mesh.devices.reshape(8, 4, 4, 2), ("z", "x", "y", "c"))
    return jax.shard_map(
        shards,
        mesh=finer,
        in_specs=(
            P(EP, None),
            P(),
            P(),
            P(None, TP),
            P(TP, None),
            P(TP, None),
            P(TP),
            P(TP, None, None),
            P(TP, None, None),
            P(TP, None, None),
            P(TP, None, None),
            P(TP),
            P(None, EP, TP),
            P(TP, None),
            P(EP, None),
            P(EP, None),
            P(EP, None, TP),
            P(EP, None, TP),
            P(EP, TP, None),
            P(TP, EP),
            P(TP, EP),
            P(EP, TP),
            P(),
        ),
        out_specs=(P(EP, TP), P(None, EP, TP)),
        check_vma=False,
    )
```
